768 devices in a mesh: sp: 96 (over z, y), tp: 8 (over x, core).
Axes of the slice: x: 4, y: 8, z: 12, core: 2. Of those that a mesh axis runs over, the one named last changes fastest.
Arguments:
- tokens: bfloat16 [12288, 2048], P(('sp', 'tp')), may hold values from -70 to 70
- w_query: bfloat16 [2048, 2048], P(None, 'tp'), may hold values from -0.1875 to 0.1875
- w_key: bfloat16 [2048, 1024], P(None, 'tp'), may hold values from -0.1875 to 0.1875
- w_value: bfloat16 [2048, 1024], P(None, 'tp'), may hold values from -0.125 to 0.125
- w_out: bfloat16 [2048, 2048], P('tp'), may hold values from -0.125 to 0.125
- lambda_head: float32 [16], P('tp'), may hold values from 0.3 to 0.8
- sub_gain: float32 [128], replicated, may hold values from 0.1 to 1.9
Outputs:
- mixed_rows: bfloat16 [12288, 2048], P(('sp', 'tp'))
The draws below stay inside these ranges and needn't reach their ends.
All inputs are finite; a program needn't handle non-finite values.
Results may differ from the reference program's by a relative error of at most 0.015.
The reference program's roundings to bfloat16 on the way count: a program that leaves them out, or rounds other values in their place, can miss the bound.
Values may be sent and summed in bfloat16 or wider, within the bound.
No kernel may reach another device: no remote copies, remote signals or barrier semaphores. Data moves between devices by JAX's collectives and lax.ppermute only.
A program may use at most 64 MiB of HBM per device.

```python
import math
import jax
import jax.numpy as jnp
from jax import lax

D = 2048
HEADS = 16
KV_HEADS = 8
QK = 64
VD = 128
TOK_DEV = 128
TOKENS = 12288
N_TP = 8


def draw_tokens(key, part):
    subkeys = jax.random.split(key, 2)
    normal_part = jnp.clip(jax.random.normal(subkeys[0], (TOKENS, D), jnp.float32), -5.0, 5.0)
    block_count = TOKENS // TOK_DEV
    offsets = jnp.clip(0.6 * jax.random.normal(subkeys[1], (block_count, D), jnp.float32), -2.0, 2.0)
    drawn = normal_part + jnp.repeat(offsets, TOK_DEV, axis=0)
    return drawn.astype(jnp.bfloat16)


def steps_of(key, dims, cuts, least, top_value):
    loudness = 1.0
    for axis_at, parts in cuts:
        draws = jax.random.uniform(jax.random.fold_in(jax.random.fold_in(key, 6), axis_at), (parts,), jnp.float32, least / len(cuts), top_value / len(cuts))
        loudness = loudness * jnp.repeat(jnp.exp(draws), dims[axis_at] // parts).reshape((-1,) + (1,) * (len(dims) - 1 - axis_at))
    return loudness


def scatter_about(own_key, dims, scale, most, cuts=(), kind=jnp.bfloat16):
    entries = scale * jax.random.normal(own_key, dims, jnp.float32)
    if cuts:
        entries = entries * steps_of(own_key, dims, cuts, -0.22, 0.18)
    return jnp.clip(entries, -most, most).astype(kind)


def setup_inputs(seed: int = 0) -> dict:
    key_of = jax.random.split(jax.random.key(seed), 8)
    return {
        "tokens": draw_tokens(jax.random.fold_in(key_of[7], 71), 0),
        "w_query": scatter_about(key_of[1], (D, HEADS * 2 * QK), (D // 2) ** -0.5, 0.1875, ((1, 8),)),
        "w_key": scatter_about(key_of[2], (D, KV_HEADS * 2 * QK), (D // 2) ** -0.5, 0.1875, ((1, 8),)),
        "w_value": scatter_about(key_of[3], (D, KV_HEADS * VD), D ** -0.5, 0.125, ((1, 8),)),
        "w_out": scatter_about(key_of[4], (HEADS * VD, D), (HEADS * VD) ** -0.5, 0.125, ((0, 8),)),
        "lambda_head": jnp.clip(0.3 + 0.5 * jax.random.uniform(key_of[5], (HEADS,), jnp.float32) ** steps_of(key_of[5], (HEADS,), ((0, 8),), -0.2, 0.2), 0.3, 0.8),
        "sub_gain": jnp.clip(1.0 + 0.18 * jax.random.normal(key_of[6], (VD,), jnp.float32), 0.1, 1.9),
    }


def reference(tokens, w_query, w_key, w_value, w_out, lambda_head, sub_gain):
    queries = jnp.dot(tokens, w_query, preferred_element_type=jnp.float32).astype(jnp.bfloat16)
    queries = queries.reshape(TOKENS, KV_HEADS, 2, 2, QK)
    keys = jnp.dot(tokens, w_key, preferred_element_type=jnp.float32).astype(jnp.bfloat16)
    keys = keys.reshape(TOKENS, KV_HEADS, 2, QK)
    values = jnp.dot(tokens, w_value, preferred_element_type=jnp.float32).astype(jnp.bfloat16)
    values = values.reshape(TOKENS, KV_HEADS, VD)
    block_rows = math.gcd(TOKENS, 512)
    block_count = TOKENS // block_rows
    key_pos = jnp.arange(TOKENS, dtype=jnp.int32)
    lambda_pair = lambda_head.reshape(KV_HEADS, 2)
    score_scale = 1.0 / math.sqrt(QK)

    def one_group(group_index):
        group_queries = lax.dynamic_index_in_dim(queries, group_index, 1, keepdims=False)
        group_keys = lax.dynamic_index_in_dim(keys, group_index, 1, keepdims=False).astype(jnp.float32)
        group_values = lax.dynamic_index_in_dim(values, group_index, 1, keepdims=False).astype(jnp.float32)
        group_lambda = lax.dynamic_index_in_dim(lambda_pair, group_index, 0, keepdims=False)

        def one_block(block_index):
            first_row = (block_index * block_rows).astype(jnp.int32)
            block_queries = lax.dynamic_slice_in_dim(group_queries, first_row, block_rows, 0).astype(jnp.float32)
            scores = jnp.einsum('tgmd,smd->gmts', block_queries, group_keys) * score_scale
            query_pos = first_row + jnp.arange(block_rows, dtype=jnp.int32)
            allowed = key_pos[None, :] <= query_pos[:, None]
            scores = jnp.where(allowed, scores, -jnp.inf)
            row_peak = lax.optimization_barrier(jnp.max(scores, axis=-1, keepdims=True))
            exponent = jnp.exp(scores - row_peak)
            row_total = lax.optimization_barrier(jnp.sum(exponent, axis=-1))
            weights = lax.optimization_barrier(exponent.astype(jnp.bfloat16)).astype(jnp.float32)
            summed = jnp.einsum('gmts,se->gmte', weights, group_values)
            normalized = summed / row_total[..., None]
            mixed_out = normalized[:, 0] - group_lambda[:, None, None] * normalized[:, 1]
            inverse_rms = lax.rsqrt(lax.optimization_barrier(jnp.mean(mixed_out * mixed_out, axis=-1, keepdims=True)) + 1e-06)
            return (mixed_out * inverse_rms * sub_gain).astype(jnp.bfloat16)
        blocks = lax.map(one_block, jnp.arange(block_count, dtype=jnp.int32))
        return jnp.transpose(blocks, (0, 2, 1, 3)).reshape(TOKENS, 2, VD)
    grouped = lax.map(one_group, jnp.arange(KV_HEADS, dtype=jnp.int32))
    heads = jnp.transpose(grouped, (1, 0, 2, 3)).reshape(TOKENS, HEADS * VD)
    group_width = HEADS * VD // N_TP

    def add_group(group_index, running):
        begin_col = (group_index * group_width).astype(jnp.int32)
        head_part = lax.dynamic_slice_in_dim(heads, begin_col, group_width, 1)
        weight_part = lax.dynamic_slice_in_dim(w_out, begin_col, group_width, 0)
        partial_out = jnp.dot(head_part, weight_part, preferred_element_type=jnp.float32).astype(jnp.bfloat16)
        return running + lax.optimization_barrier(partial_out).astype(jnp.float32)
    summed_out = lax.fori_loop(0, N_TP, add_group, jnp.zeros((TOKENS, D), jnp.float32))
    return summed_out.astype(jnp.bfloat16)
```

```python
import functools
import math

import jax
import jax.numpy as jnp
from jax import lax
from jax.experimental import pallas as pl
from jax.experimental.pallas import tpu as pltpu
from jax.sharding import Mesh, PartitionSpec as P

QK = 64
VD = 128
BLOCK = 128
Y = 8
STAT_ROWS = 16
SEND_ROWS = 2 * VD + STAT_ROWS
EMPTY = -1e30
HIDDEN = -2e38
BASE2_SCALE = math.log2(math.e) / math.sqrt(QK)

VMEM = pl.BlockSpec(memory_space=pltpu.VMEM)
SMEM = pl.BlockSpec(memory_space=pltpu.SMEM)


def three_parts(value):
    high = value.astype(jnp.bfloat16)
    rest = value - high.astype(jnp.float32)
    middle = rest.astype(jnp.bfloat16)
    low = (rest - middle.astype(jnp.float32)).astype(jnp.bfloat16)
    return [part.astype(jnp.float32) for part in (high, middle, low)]


def attend_block(row_blocks, place_ref, q_ref, kv_ref, out_ref, b):
    z, y = place_ref[0], place_ref[1]
    q_block = q_ref[b]
    q_rows = jnp.concatenate([q_block[:, : 2 * QK], q_block[:, 2 * QK :]], axis=0)
    lane = lax.broadcasted_iota(jnp.int32, q_rows.shape, 1)
    k_rows = jnp.concatenate([kv_ref[i, :BLOCK, :] for i in range(row_blocks)], axis=0)
    v_cols = jnp.concatenate([kv_ref[i, BLOCK:, :] for i in range(row_blocks)], axis=1)
    span = row_blocks * BLOCK
    masked = 4 * BLOCK
    r = lax.broadcasted_iota(jnp.int32, (masked, 2 * BLOCK), 0)
    c = lax.broadcasted_iota(jnp.int32, (masked, 2 * BLOCK), 1)
    key_pos = ((r // BLOCK + (row_blocks - 4)) * Y + y) * BLOCK + r % BLOCK
    query_pos = (z * Y + b) * BLOCK + c % BLOCK
    allowed = key_pos <= query_pos
    stats = []
    for m in range(2):
        q_map = jnp.where((lane >= QK) == (m == 1), q_rows, jnp.zeros_like(q_rows))
        scores = lax.dot_general(
            k_rows, q_map, (((1,), (1,)), ((), ())), preferred_element_type=jnp.float32
        )
        tail = jnp.where(allowed, scores[span - masked :], HIDDEN)
        if span > masked:
            scores = jnp.concatenate([scores[: span - masked], tail], axis=0)
        else:
            scores = tail
        peak = jnp.maximum(jnp.max(scores, axis=0, keepdims=True), EMPTY)
        expo = jnp.exp2((scores - peak) * BASE2_SCALE)
        total = jnp.sum(expo, axis=0, keepdims=True)
        summed = jnp.dot(
            v_cols, expo.astype(jnp.bfloat16), preferred_element_type=jnp.float32
        )
        inverse = jnp.where(total > 0.0, 1.0 / total, 0.0)
        out_ref[b, m * VD : (m + 1) * VD, :] = (summed * inverse).astype(jnp.bfloat16)
        stats += three_parts(peak) + three_parts(total)
    stats += [jnp.zeros_like(stats[0])] * (STAT_ROWS - len(stats))
    out_ref[b, 2 * VD :, :] = jnp.concatenate(stats, axis=0).astype(jnp.bfloat16)


def attend_kernel(place_ref, q_ref, kv_ref, out_ref):
    z = place_ref[0]
    rows = kv_ref.shape[0]
    for row_blocks in range(4, rows + 1, 4):

        @pl.when((z >= row_blocks - 4) & (z < row_blocks))
        def _():
            @pl.loop(0, Y)
            def _(b):
                attend_block(row_blocks, place_ref, q_ref, kv_ref, out_ref, b)


def attend(place, queries, key_values):
    return pl.pallas_call(
        attend_kernel,
        out_shape=jax.ShapeDtypeStruct((Y, SEND_ROWS, 2 * BLOCK), jnp.bfloat16),
        in_specs=[SMEM, VMEM, VMEM],
        out_specs=VMEM,
        cost_estimate=pl.CostEstimate(
            flops=4_000_000_000, bytes_accessed=3_000_000, transcendentals=6_000_000
        ),
        name="attend",
    )(place, queries, key_values)


def merge_kernel(part_ref, lambda_ref, gain_ref, w_ref, out_ref):
    stats = [part_ref[s, 2 * VD :, :].astype(jnp.float32) for s in range(Y)]
    mixed = None
    for m in range(2):
        at = 6 * m
        peaks = [s[at : at + 1] + s[at + 1 : at + 2] + s[at + 2 : at + 3] for s in stats]
        totals = [s[at + 3 : at + 4] + s[at + 4 : at + 5] + s[at + 5 : at + 6] for s in stats]
        top = functools.reduce(jnp.maximum, peaks)
        shares = [jnp.exp2((p - top) * BASE2_SCALE) * t for p, t in zip(peaks, totals)]
        inverse = 1.0 / sum(shares)
        normalized = sum(
            part_ref[s, m * VD : (m + 1) * VD, :].astype(jnp.float32) * (shares[s] * inverse)
            for s in range(Y)
        )
        if m == 0:
            mixed = normalized
        else:
            column = lax.broadcasted_iota(jnp.int32, (1, 2 * BLOCK), 1)
            head_lambda = jnp.where(column < BLOCK, lambda_ref[0], lambda_ref[1])
            mixed = mixed - head_lambda * normalized
    inverse_rms = lax.rsqrt(jnp.mean(mixed * mixed, axis=0, keepdims=True) + 1e-06)
    heads = mixed * inverse_rms * gain_ref[...]
    rows = jnp.concatenate([heads[:, :BLOCK].T, heads[:, BLOCK:].T], axis=1)
    out_ref[...] = jnp.dot(
        rows.astype(jnp.bfloat16), w_ref[...], preferred_element_type=jnp.float32
    ).astype(jnp.bfloat16)


def merge(parts, lambda_head, sub_gain, w_out):
    return pl.pallas_call(
        merge_kernel,
        out_shape=jax.ShapeDtypeStruct((BLOCK, w_out.shape[1]), jnp.bfloat16),
        in_specs=[VMEM, SMEM, VMEM, VMEM],
        out_specs=VMEM,
        name="merge",
    )(parts, lambda_head, sub_gain.reshape(VD, 1), w_out)


def to_everyone(value, axis):
    length = lax.axis_size(axis)
    return lax.all_to_all(
        jnp.broadcast_to(value[None], (length, *value.shape)), axis, 0, 0, tiled=True
    )


def body(tokens, w_query, w_key, w_value, w_out, lambda_head, sub_gain):
    tp = lax.axis_size("tp")
    rows = to_everyone(tokens, "tp").reshape(tp * tokens.shape[0], tokens.shape[1])
    dot = functools.partial(lax.dot_general, preferred_element_type=jnp.float32)
    queries = dot(rows, w_query, (((1,), (0,)), ((), ()))).astype(jnp.bfloat16)
    keys = dot(rows, w_key, (((1,), (0,)), ((), ()))).astype(jnp.bfloat16)
    values = dot(w_value, rows, (((0,), (1,)), ((), ()))).astype(jnp.bfloat16)
    all_queries = to_everyone(queries, "y")
    key_values = lax.all_gather(jnp.concatenate([keys, values], axis=0), "z")
    place = jnp.stack([lax.axis_index("z"), lax.axis_index("y")]).astype(jnp.int32)
    parts = attend(place, all_queries, key_values)
    parts = lax.all_to_all(parts, "y", 0, 0, tiled=True)
    partial_rows = merge(parts, lambda_head, sub_gain, w_out)
    arrived = lax.all_to_all(
        partial_rows.reshape(tp, -1, partial_rows.shape[1]), "tp", 0, 0, tiled=True
    )
    return arrived.astype(jnp.float32).sum(axis=0).astype(jnp.bfloat16)


def solution(mesh):
    sp, tp = mesh.devices.shape
    grid = Mesh(mesh.devices.reshape(sp // Y, Y, tp), ("z", "y", "tp"))
    everyone = ("z", "y", "tp")
    return jax.shard_map(
        body,
        mesh=grid,
        in_specs=(
            P(everyone, None),
            P(None, "tp"),
            P(None, "tp"),
            P(None, "tp"),
            P("tp", None),
            P("tp"),
            P(),
        ),
        out_specs=P(everyone, None),
        check_vma=False,
    )
```

```python
import functools
import math

import jax
import jax.numpy as jnp
from jax import lax
from jax.experimental import pallas as pl
from jax.experimental.pallas import tpu as pltpu
from jax.sharding import Mesh, PartitionSpec as P

QK = 64
VD = 128
BLOCK = 128
TILE = 2 * BLOCK
Y = 8
STAT_ROWS = 16
SEND_ROWS = 2 * VD + STAT_ROWS
EMPTY = -1e30
HIDDEN = -2e38
BASE2_SCALE = math.log2(math.e) / math.sqrt(QK)
CASES = ((0, 3, 4, 4), (4, 7, 8, 4), (8, 10, 11, 3), (11, 11, 12, 1))

VMEM = pl.BlockSpec(memory_space=pltpu.VMEM)
SMEM = pl.BlockSpec(memory_space=pltpu.SMEM)


def three_parts(value):
    high = value.astype(jnp.bfloat16)
    rest = value - high.astype(jnp.float32)
    middle = rest.astype(jnp.bfloat16)
    low = (rest - middle.astype(jnp.float32)).astype(jnp.bfloat16)
    return [part.astype(jnp.float32) for part in (high, middle, low)]


def folded(op, value):
    return op(value.reshape(value.shape[0] // 8, 8, value.shape[1]), axis=0)


def score_pass(blocks, tail, place, q_ref, k_refs, b, offsets, score_refs):
    z, y = place
    q_block = q_ref[b]
    q_rows = jnp.concatenate([q_block[:, : 2 * QK], q_block[:, 2 * QK :]], axis=0)
    q_scaled = q_rows.astype(jnp.float32) * BASE2_SCALE
    high = q_scaled.astype(jnp.bfloat16)
    low = (q_scaled - high.astype(jnp.float32)).astype(jnp.bfloat16)
    peaks = []
    for m in range(2):
        lanes = slice(m * QK, (m + 1) * QK)
        q_map = jnp.concatenate([high[:, lanes], low[:, lanes]], axis=1)
        scores = lax.dot_general(
            k_refs[m][: blocks * BLOCK, :],
            q_map,
            (((1,), (1,)), ((), ())),
            preferred_element_type=jnp.float32,
        )
        top = jnp.full((8, TILE), EMPTY, jnp.float32)
        for block in range(blocks):
            rows = slice(block * BLOCK, (block + 1) * BLOCK)
            part = scores[rows]
            if block >= blocks - tail:
                reach = (z - block) * (Y * BLOCK) + (b - y) * BLOCK
                part = jnp.where(offsets <= reach, part, HIDDEN)
            score_refs[m][rows, :] = part
            top = jnp.maximum(top, folded(jnp.max, part))
        peaks.append(jnp.max(top, axis=0, keepdims=True))
    return peaks


def value_pass(blocks, v_ref, out_ref, b, score_refs, weight_refs, peaks):
    stats = []
    for m in range(2):
        peak = peaks[m]
        running = jnp.zeros((8, TILE), jnp.float32)
        for block in range(blocks):
            rows = slice(block * BLOCK, (block + 1) * BLOCK)
            expo = jnp.exp2(score_refs[m][rows, :] - peak)
            running = running + folded(jnp.sum, expo)
            weight_refs[m][rows, :] = expo.astype(jnp.bfloat16)
        total = jnp.sum(running, axis=0, keepdims=True)
        summed = jnp.dot(
            v_ref[:, : blocks * BLOCK],
            weight_refs[m][: blocks * BLOCK, :],
            preferred_element_type=jnp.float32,
        )
        inverse = jnp.where(total > 0.0, 1.0 / total, 0.0)
        out_ref[b, m * VD : (m + 1) * VD, :] = (summed * inverse).astype(jnp.bfloat16)
        stats += three_parts(peak) + three_parts(total)
    stats += [jnp.zeros_like(stats[0])] * (STAT_ROWS - len(stats))
    out_ref[b, 2 * VD :, :] = jnp.concatenate(stats, axis=0).astype(jnp.bfloat16)


def attend_kernel(place_ref, q_ref, kv_ref, out_ref, v_ref, k0_ref, k1_ref, *scratch):
    z, y = place_ref[0], place_ref[1]
    for block in range(kv_ref.shape[0]):
        rows = slice(block * BLOCK, (block + 1) * BLOCK)
        v_ref[:, rows] = kv_ref[block, BLOCK:, :]
        k = kv_ref[block, :BLOCK, :]
        k0_ref[rows, :] = jnp.concatenate([k[:, :QK], k[:, :QK]], axis=1)
        k1_ref[rows, :] = jnp.concatenate([k[:, QK:], k[:, QK:]], axis=1)
    key_row = lax.broadcasted_iota(jnp.int32, (BLOCK, TILE), 0)
    query_row = lax.rem(lax.broadcasted_iota(jnp.int32, (BLOCK, TILE), 1), BLOCK)
    offsets = key_row - query_row
    scores = (scratch[0:2], scratch[2:4])
    weights = (scratch[4:6], scratch[6:8])
    for low, high, blocks, tail in CASES:

        @pl.when((z >= low) & (z <= high))
        def _():
            def score(b, slot):
                return score_pass(
                    blocks, tail, (z, y), q_ref, (k0_ref, k1_ref), b, offsets, scores[slot]
                )

            def value(b, slot, peaks):
                value_pass(blocks, v_ref, out_ref, b, scores[slot], weights[slot], peaks)

            def two(i, peaks, more=True):
                odd = score(2 * i + 1, 1)
                value(2 * i, 0, peaks)
                even = score(2 * i + 2, 0) if more else None
                value(2 * i + 1, 1, odd)
                return even

            last = Y // 2 - 1
            two(last, lax.fori_loop(0, last, two, score(0, 0)), False)


def attend(place, queries, key_values):
    span = key_values.shape[0] * BLOCK
    return pl.pallas_call(
        attend_kernel,
        out_shape=jax.ShapeDtypeStruct((Y, SEND_ROWS, TILE), jnp.bfloat16),
        in_specs=[SMEM, VMEM, VMEM],
        out_specs=VMEM,
        scratch_shapes=[pltpu.VMEM((VD, span), jnp.bfloat16)]
        + [pltpu.VMEM((span, 2 * QK), jnp.bfloat16)] * 2
        + [pltpu.VMEM((span, TILE), jnp.float32)] * 4
        + [pltpu.VMEM((span, TILE), jnp.bfloat16)] * 4,
        compiler_params=pltpu.CompilerParams(vmem_limit_bytes=20 * 2**20),
        cost_estimate=pl.CostEstimate(
            flops=4_000_000_000, bytes_accessed=3_000_000, transcendentals=6_000_000
        ),
        name="attend",
    )(place, queries, key_values)


def merge_kernel(part_ref, lambda_ref, gain_ref, w_ref, out_ref):
    stats = [part_ref[s, 2 * VD :, :].astype(jnp.float32) for s in range(Y)]
    both = []
    for m in range(2):
        at = 6 * m
        peaks = [s[at : at + 1] + s[at + 1 : at + 2] + s[at + 2 : at + 3] for s in stats]
        totals = [s[at + 3 : at + 4] + s[at + 4 : at + 5] + s[at + 5 : at + 6] for s in stats]
        top = functools.reduce(jnp.maximum, peaks)
        shares = [jnp.exp2(p - top) * t for p, t in zip(peaks, totals)]
        inverse = 1.0 / sum(shares)
        both.append(
            sum(
                part_ref[s, m * VD : (m + 1) * VD, :].astype(jnp.float32) * (shares[s] * inverse)
                for s in range(Y)
            )
        )
    column = lax.broadcasted_iota(jnp.int32, (1, TILE), 1)
    mixed = both[0] - jnp.where(column < BLOCK, lambda_ref[0], lambda_ref[1]) * both[1]
    inverse_rms = lax.rsqrt(jnp.mean(mixed * mixed, axis=0, keepdims=True) + 1e-06)
    heads = mixed * inverse_rms * gain_ref[...]
    rows = jnp.concatenate([heads[:, :BLOCK].T, heads[:, BLOCK:].T], axis=1)
    out_ref[...] = jnp.dot(
        rows.astype(jnp.bfloat16), w_ref[...], preferred_element_type=jnp.float32
    ).astype(jnp.bfloat16)


def merge(parts, lambda_head, sub_gain, w_out):
    return pl.pallas_call(
        merge_kernel,
        out_shape=jax.ShapeDtypeStruct((BLOCK, w_out.shape[1]), jnp.bfloat16),
        in_specs=[VMEM, SMEM, VMEM, VMEM],
        out_specs=VMEM,
        compiler_params=pltpu.CompilerParams(vmem_limit_bytes=12 * 2**20),
        cost_estimate=pl.CostEstimate(
            flops=1_000_000_000, bytes_accessed=3_000_000, transcendentals=8_000
        ),
        name="merge",
    )(parts, lambda_head, sub_gain.reshape(VD, 1), w_out)


def to_everyone(value, axis):
    length = lax.axis_size(axis)
    return lax.all_to_all(
        jnp.broadcast_to(value[None], (length, *value.shape)), axis, 0, 0, tiled=True
    )


def body(tokens, w_query, w_key, w_value, w_out, lambda_head, sub_gain):
    tp = lax.axis_size("tp")
    rows = lax.all_gather(tokens, "tp", axis=0, tiled=True)
    dot = functools.partial(lax.dot_general, preferred_element_type=jnp.float32)
    queries = dot(rows, w_query, (((1,), (0,)), ((), ()))).astype(jnp.bfloat16)
    keys = dot(rows, w_key, (((1,), (0,)), ((), ()))).astype(jnp.bfloat16)
    values = dot(w_value, rows, (((0,), (1,)), ((), ()))).astype(jnp.bfloat16)
    all_queries = to_everyone(queries, "y")
    key_values = lax.all_gather(jnp.concatenate([keys, values], axis=0), "z")
    place = jnp.stack([lax.axis_index("z"), lax.axis_index("y")]).astype(jnp.int32)
    parts = attend(place, all_queries, key_values)
    parts = lax.all_to_all(parts, "y", 0, 0, tiled=True)
    partial_rows = merge(parts, lambda_head, sub_gain, w_out)
    arrived = lax.all_to_all(
        partial_rows.reshape(tp, -1, partial_rows.shape[1]), "tp", 0, 0, tiled=True
    )
    return arrived.astype(jnp.float32).sum(axis=0).astype(jnp.bfloat16)


def solution(mesh):
    sp, tp = mesh.devices.shape
    grid = Mesh(mesh.devices.reshape(sp // Y, Y, tp), ("z", "y", "tp"))
    everyone = ("z", "y", "tp")
    return jax.shard_map(
        body,
        mesh=grid,
        in_specs=(
            P(everyone, None),
            P(None, "tp"),
            P(None, "tp"),
            P(None, "tp"),
            P("tp", None),
            P("tp"),
            P(),
        ),
        out_specs=P(everyone, None),
        check_vma=False,
    )
```

```python
import functools
import math

import jax
import jax.numpy as jnp
from jax import lax
from jax.experimental import pallas as pl
from jax.experimental.pallas import tpu as pltpu
from jax.sharding import Mesh, PartitionSpec as P

QK = 64
VD = 128
BLOCK = 128
TILE = 2 * BLOCK
Y = 8
STAT_ROWS = 16
SEND_ROWS = 2 * VD + STAT_ROWS
EMPTY = -1e30
HIDDEN = -2e38
BASE2_SCALE = math.log2(math.e) / math.sqrt(QK)
CASES = ((0, 0, 1), (1, 1, 2), (2, 2, 3), (3, 4, 5), (5, 7, 8), (8, 10, 11), (11, 11, 12))
CHUNK = 2

VMEM = pl.BlockSpec(memory_space=pltpu.VMEM)
SMEM = pl.BlockSpec(memory_space=pltpu.SMEM)


def three_parts(value):
    high = value.astype(jnp.bfloat16)
    rest = value - high.astype(jnp.float32)
    middle = rest.astype(jnp.bfloat16)
    low = (rest - middle.astype(jnp.float32)).astype(jnp.bfloat16)
    return [part.astype(jnp.float32) for part in (high, middle, low)]


def folded(op, value):
    return op(value.reshape(value.shape[0] // 8, 8, value.shape[1]), axis=0)


def both_maps(q_ref, b):
    q_block = q_ref[b]
    q_rows = jnp.concatenate([q_block[:, : 2 * QK], q_block[:, 2 * QK :]], axis=0)
    q_scaled = q_rows.astype(jnp.float32) * BASE2_SCALE
    high = q_scaled.astype(jnp.bfloat16)
    low = (q_scaled - high.astype(jnp.float32)).astype(jnp.bfloat16)
    return [
        jnp.concatenate([high[:, m * QK : (m + 1) * QK], low[:, m * QK : (m + 1) * QK]], axis=1)
        for m in range(2)
    ]


def attend_kernel(place_ref, q_ref, kv_ref, out_ref, v_ref, k0_ref, k1_ref, *scratch):
    z, y = place_ref[0], place_ref[1]
    k_refs = (k0_ref, k1_ref)
    slots = (scratch[0:2], scratch[2:4])
    key_row = lax.broadcasted_iota(jnp.int32, (BLOCK, TILE), 0)
    query_row = lax.rem(lax.broadcasted_iota(jnp.int32, (BLOCK, TILE), 1), BLOCK)
    offsets = key_row - query_row

    def step(case, later, slot_later, now, slot_now, peaks):
        low, _, blocks = case
        if later is not None:
            queries = both_maps(q_ref, later)
            tops = [jnp.full((8, TILE), EMPTY, jnp.float32) for _ in range(2)]
        if now is not None:
            totals = [jnp.zeros((8, TILE), jnp.float32) for _ in range(2)]
            summed = [0.0, 0.0]
        for first in range(0, blocks, CHUNK):
            last = min(first + CHUNK, blocks)
            rows = slice(first * BLOCK, last * BLOCK)
            for m in range(2):
                if later is not None:
                    scores = lax.dot_general(
                        k_refs[m][rows, :],
                        queries[m],
                        (((1,), (1,)), ((), ())),
                        preferred_element_type=jnp.float32,
                    )
                    for block in range(first, last):
                        part = scores[(block - first) * BLOCK : (block - first + 1) * BLOCK]
                        if block >= low:
                            reach = (z - block) * (Y * BLOCK) + (later - y) * BLOCK
                            part = jnp.where(offsets <= reach, part, HIDDEN)
                        slots[slot_later][m][block * BLOCK : (block + 1) * BLOCK, :] = part
                        tops[m] = jnp.maximum(tops[m], folded(jnp.max, part))
                if now is not None:
                    expo = jnp.exp2(slots[slot_now][m][rows, :] - peaks[m])
                    totals[m] = totals[m] + folded(jnp.sum, expo)
                    summed[m] = summed[m] + jnp.dot(
                        v_ref[:, rows], expo.astype(jnp.bfloat16), preferred_element_type=jnp.float32
                    )
        if now is not None:
            stats = []
            for m in range(2):
                total = jnp.sum(totals[m], axis=0, keepdims=True)
                inverse = jnp.where(total > 0.0, 1.0 / total, 0.0)
                out_ref[now, m * VD : (m + 1) * VD, :] = (summed[m] * inverse).astype(jnp.bfloat16)
                stats += three_parts(peaks[m]) + three_parts(total)
            stats += [jnp.zeros_like(stats[0])] * (STAT_ROWS - len(stats))
            out_ref[now, 2 * VD :, :] = jnp.concatenate(stats, axis=0).astype(jnp.bfloat16)
        if later is not None:
            return [jnp.max(top, axis=0, keepdims=True) for top in tops]
        return None

    for case in CASES:

        @pl.when((z >= case[0]) & (z <= case[1]))
        def _():
            for block in range(case[2]):
                rows = slice(block * BLOCK, (block + 1) * BLOCK)
                v_ref[:, rows] = kv_ref[block, BLOCK:, :]
                k = kv_ref[block, :BLOCK, :]
                k0_ref[rows, :] = jnp.concatenate([k[:, :QK], k[:, :QK]], axis=1)
                k1_ref[rows, :] = jnp.concatenate([k[:, QK:], k[:, QK:]], axis=1)

            def two(i, peaks, more=True):
                odd = step(case, 2 * i + 1, 1, 2 * i, 0, peaks)
                return step(case, 2 * i + 2 if more else None, 0, 2 * i + 1, 1, odd)

            end = Y // 2 - 1
            two(end, lax.fori_loop(0, end, two, step(case, 0, 0, None, 1, None)), False)


def attend(place, queries, key_values):
    span = key_values.shape[0] * BLOCK
    return pl.pallas_call(
        attend_kernel,
        out_shape=jax.ShapeDtypeStruct((Y, SEND_ROWS, TILE), jnp.bfloat16),
        in_specs=[SMEM, VMEM, VMEM],
        out_specs=VMEM,
        scratch_shapes=[pltpu.VMEM((VD, span), jnp.bfloat16)]
        + [pltpu.VMEM((span, 2 * QK), jnp.bfloat16)] * 2
        + [pltpu.VMEM((span, TILE), jnp.float32)] * 4,
        compiler_params=pltpu.CompilerParams(vmem_limit_bytes=16 * 2**20),
        cost_estimate=pl.CostEstimate(
            flops=4_000_000_000, bytes_accessed=3_000_000, transcendentals=6_000_000
        ),
        name="attend",
    )(place, queries, key_values)


def merge_kernel(part_ref, lambda_ref, gain_ref, w_ref, out_ref):
    stats = [part_ref[s, 2 * VD :, :].astype(jnp.float32) for s in range(Y)]
    both = []
    for m in range(2):
        at = 6 * m
        peaks = [s[at : at + 1] + s[at + 1 : at + 2] + s[at + 2 : at + 3] for s in stats]
        totals = [s[at + 3 : at + 4] + s[at + 4 : at + 5] + s[at + 5 : at + 6] for s in stats]
        top = functools.reduce(jnp.maximum, peaks)
        shares = [jnp.exp2(p - top) * t for p, t in zip(peaks, totals)]
        inverse = 1.0 / sum(shares)
        both.append(
            sum(
                part_ref[s, m * VD : (m + 1) * VD, :].astype(jnp.float32) * (shares[s] * inverse)
                for s in range(Y)
            )
        )
    column = lax.broadcasted_iota(jnp.int32, (1, TILE), 1)
    mixed = both[0] - jnp.where(column < BLOCK, lambda_ref[0], lambda_ref[1]) * both[1]
    inverse_rms = lax.rsqrt(jnp.mean(mixed * mixed, axis=0, keepdims=True) + 1e-06)
    heads = mixed * inverse_rms * gain_ref[...]
    rows = jnp.concatenate([heads[:, :BLOCK].T, heads[:, BLOCK:].T], axis=1)
    out_ref[...] = jnp.dot(
        rows.astype(jnp.bfloat16), w_ref[...], preferred_element_type=jnp.float32
    ).astype(jnp.bfloat16)


def merge(parts, lambda_head, sub_gain, w_out):
    return pl.pallas_call(
        merge_kernel,
        out_shape=jax.ShapeDtypeStruct((BLOCK, w_out.shape[1]), jnp.bfloat16),
        in_specs=[VMEM, SMEM, VMEM, VMEM],
        out_specs=VMEM,
        compiler_params=pltpu.CompilerParams(vmem_limit_bytes=12 * 2**20),
        cost_estimate=pl.CostEstimate(
            flops=1_000_000_000, bytes_accessed=3_000_000, transcendentals=8_000
        ),
        name="merge",
    )(parts, lambda_head, sub_gain.reshape(VD, 1), w_out)


def to_everyone(value, axis):
    length = lax.axis_size(axis)
    return lax.all_to_all(
        jnp.broadcast_to(value[None], (length, *value.shape)), axis, 0, 0, tiled=True
    )


def body(tokens, w_query, w_key, w_value, w_out, lambda_head, sub_gain):
    tp = lax.axis_size("tp")
    rows = lax.all_gather(tokens, "tp", axis=0, tiled=True)
    dot = functools.partial(lax.dot_general, preferred_element_type=jnp.float32)
    queries = dot(rows, w_query, (((1,), (0,)), ((), ()))).astype(jnp.bfloat16)
    keys = dot(rows, w_key, (((1,), (0,)), ((), ()))).astype(jnp.bfloat16)
    values = dot(w_value, rows, (((0,), (1,)), ((), ()))).astype(jnp.bfloat16)
    all_queries = to_everyone(queries, "y")
    key_values = lax.all_gather(jnp.concatenate([keys, values], axis=0), "z")
    place = jnp.stack([lax.axis_index("z"), lax.axis_index("y")]).astype(jnp.int32)
    parts = attend(place, all_queries, key_values)
    parts = lax.all_to_all(parts, "y", 0, 0, tiled=True)
    partial_rows = merge(parts, lambda_head, sub_gain, w_out)
    arrived = lax.all_to_all(
        partial_rows.reshape(tp, -1, partial_rows.shape[1]), "tp", 0, 0, tiled=True
    )
    return arrived.astype(jnp.float32).sum(axis=0).astype(jnp.bfloat16)


def solution(mesh):
    sp, tp = mesh.devices.shape
    grid = Mesh(mesh.devices.reshape(sp // Y, Y, tp), ("z", "y", "tp"))
    everyone = ("z", "y", "tp")
    return jax.shard_map(
        body,
        mesh=grid,
        in_specs=(
            P(everyone, None),
            P(None, "tp"),
            P(None, "tp"),
            P(None, "tp"),
            P("tp", None),
            P("tp"),
            P(),
        ),
        out_specs=P(everyone, None),
        check_vma=False,
    )
```

```python
import functools
import math

import jax
import jax.numpy as jnp
from jax import lax
from jax.experimental import pallas as pl
from jax.experimental.pallas import tpu as pltpu
from jax.sharding import Mesh, PartitionSpec as P

QK = 64
VD = 128
BLOCK = 128
TILE = 2 * BLOCK
Y = 8
STAT_ROWS = 8
SEND_ROWS = 2 * VD + STAT_ROWS
EMPTY = -1e30
HIDDEN = -2e38
BASE2_SCALE = math.log2(math.e) / math.sqrt(QK)
CASES = ((0, 0, 1), (1, 1, 2), (2, 2, 3), (3, 4, 5), (5, 7, 8), (8, 10, 11), (11, 11, 12))
CHUNK = 2

VMEM = pl.BlockSpec(memory_space=pltpu.VMEM)
SMEM = pl.BlockSpec(memory_space=pltpu.SMEM)


def three_parts(value):
    high = value.astype(jnp.bfloat16)
    rest = value - high.astype(jnp.float32)
    middle = rest.astype(jnp.bfloat16)
    low = (rest - middle.astype(jnp.float32)).astype(jnp.bfloat16)
    return [part.astype(jnp.float32) for part in (high, middle, low)]


def folded(op, value):
    return op(value.reshape(value.shape[0] // 8, 8, value.shape[1]), axis=0)


def both_maps(q_ref, b):
    q_block = q_ref[b]
    q_rows = jnp.concatenate([q_block[:, : 2 * QK], q_block[:, 2 * QK :]], axis=0)
    q_scaled = q_rows.astype(jnp.float32) * BASE2_SCALE
    high = q_scaled.astype(jnp.bfloat16)
    low = (q_scaled - high.astype(jnp.float32)).astype(jnp.bfloat16)
    return [
        jnp.concatenate([high[:, m * QK : (m + 1) * QK], low[:, m * QK : (m + 1) * QK]], axis=1)
        for m in range(2)
    ]


def attend_kernel(place_ref, q_ref, kv_ref, out_ref, v_ref, k0_ref, k1_ref, *scratch):
    z, y = place_ref[0], place_ref[1]
    k_refs = (k0_ref, k1_ref)
    slots = (scratch[0:2], scratch[2:4])
    key_row = lax.broadcasted_iota(jnp.int32, (BLOCK, TILE), 0)
    query_row = lax.rem(lax.broadcasted_iota(jnp.int32, (BLOCK, TILE), 1), BLOCK)
    offsets = key_row - query_row

    def step(case, later, slot_later, now, slot_now, peaks):
        low, _, blocks = case
        if later is not None:
            queries = both_maps(q_ref, later)
            tops = [jnp.full((8, TILE), EMPTY, jnp.float32) for _ in range(2)]
        if now is not None:
            totals = [jnp.zeros((8, TILE), jnp.float32) for _ in range(2)]
            summed = [0.0, 0.0]
        for first in range(0, blocks, CHUNK):
            last = min(first + CHUNK, blocks)
            rows = slice(first * BLOCK, last * BLOCK)
            for m in range(2):
                if later is not None:
                    scores = lax.dot_general(
                        k_refs[m][rows, :],
                        queries[m],
                        (((1,), (1,)), ((), ())),
                        preferred_element_type=jnp.float32,
                    )
                    for block in range(first, last):
                        part = scores[(block - first) * BLOCK : (block - first + 1) * BLOCK]
                        if block >= low:
                            reach = (z - block) * (Y * BLOCK) + (later - y) * BLOCK
                            part = jnp.where(offsets <= reach, part, HIDDEN)
                        slots[slot_later][m][block * BLOCK : (block + 1) * BLOCK, :] = part
                        tops[m] = jnp.maximum(tops[m], folded(jnp.max, part))
                if now is not None:
                    expo = jnp.exp2(slots[slot_now][m][rows, :] - peaks[m])
                    totals[m] = totals[m] + folded(jnp.sum, expo)
                    summed[m] = summed[m] + jnp.dot(
                        v_ref[:, rows], expo.astype(jnp.bfloat16), preferred_element_type=jnp.float32
                    )
        if now is not None:
            stats = []
            for m in range(2):
                total = jnp.sum(totals[m], axis=0, keepdims=True)
                total = total.astype(jnp.bfloat16).astype(jnp.float32)
                inverse = jnp.where(total > 0.0, 1.0 / total, 0.0)
                out_ref[now, m * VD : (m + 1) * VD, :] = (summed[m] * inverse).astype(jnp.bfloat16)
                stats += three_parts(peaks[m]) + [total]
            out_ref[now, 2 * VD :, :] = jnp.concatenate(stats, axis=0).astype(jnp.bfloat16)
        if later is not None:
            return [jnp.max(top, axis=0, keepdims=True) for top in tops]
        return None

    for case in CASES:

        @pl.when((z >= case[0]) & (z <= case[1]))
        def _():
            for block in range(case[2]):
                rows = slice(block * BLOCK, (block + 1) * BLOCK)
                v_ref[:, rows] = kv_ref[block, BLOCK:, :]
                k = kv_ref[block, :BLOCK, :]
                k0_ref[rows, :] = jnp.concatenate([k[:, :QK], k[:, :QK]], axis=1)
                k1_ref[rows, :] = jnp.concatenate([k[:, QK:], k[:, QK:]], axis=1)

            def two(i, peaks, more=True):
                odd = step(case, 2 * i + 1, 1, 2 * i, 0, peaks)
                return step(case, 2 * i + 2 if more else None, 0, 2 * i + 1, 1, odd)

            end = Y // 2 - 1
            two(end, lax.fori_loop(0, end, two, step(case, 0, 0, None, 1, None)), False)


def attend(place, queries, key_values):
    span = key_values.shape[0] * BLOCK
    return pl.pallas_call(
        attend_kernel,
        out_shape=jax.ShapeDtypeStruct((Y, SEND_ROWS, TILE), jnp.bfloat16),
        in_specs=[SMEM, VMEM, VMEM],
        out_specs=VMEM,
        scratch_shapes=[pltpu.VMEM((VD, span), jnp.bfloat16)]
        + [pltpu.VMEM((span, 2 * QK), jnp.bfloat16)] * 2
        + [pltpu.VMEM((span, TILE), jnp.float32)] * 4,
        compiler_params=pltpu.CompilerParams(vmem_limit_bytes=16 * 2**20),
        cost_estimate=pl.CostEstimate(
            flops=4_000_000_000, bytes_accessed=3_000_000, transcendentals=6_000_000
        ),
        name="attend",
    )(place, queries, key_values)


def merge_kernel(part_ref, lambda_ref, gain_ref, w_ref, out_ref):
    stats = [part_ref[s, 2 * VD :, :].astype(jnp.float32) for s in range(Y)]
    both = []
    for m in range(2):
        at = 4 * m
        peaks = [s[at : at + 1] + s[at + 1 : at + 2] + s[at + 2 : at + 3] for s in stats]
        totals = [s[at + 3 : at + 4] for s in stats]
        top = functools.reduce(jnp.maximum, peaks)
        shares = [jnp.exp2(p - top) * t for p, t in zip(peaks, totals)]
        inverse = 1.0 / sum(shares)
        both.append(
            sum(
                part_ref[s, m * VD : (m + 1) * VD, :].astype(jnp.float32) * (shares[s] * inverse)
                for s in range(Y)
            )
        )
    column = lax.broadcasted_iota(jnp.int32, (1, TILE), 1)
    mixed = both[0] - jnp.where(column < BLOCK, lambda_ref[0], lambda_ref[1]) * both[1]
    inverse_rms = lax.rsqrt(jnp.mean(mixed * mixed, axis=0, keepdims=True) + 1e-06)
    heads = mixed * inverse_rms
    rows = [heads[:, h * BLOCK : (h + 1) * BLOCK].T * gain_ref[...] for h in range(2)]
    rows = jnp.concatenate(rows, axis=1)
    out_ref[...] = jnp.dot(
        rows.astype(jnp.bfloat16), w_ref[...], preferred_element_type=jnp.float32
    ).astype(jnp.bfloat16)


def merge(parts, lambda_head, sub_gain, w_out):
    return pl.pallas_call(
        merge_kernel,
        out_shape=jax.ShapeDtypeStruct((BLOCK, w_out.shape[1]), jnp.bfloat16),
        in_specs=[VMEM, SMEM, VMEM, VMEM],
        out_specs=VMEM,
        compiler_params=pltpu.CompilerParams(vmem_limit_bytes=12 * 2**20),
        cost_estimate=pl.CostEstimate(
            flops=1_000_000_000, bytes_accessed=3_000_000, transcendentals=8_000
        ),
        name="merge",
    )(parts, lambda_head, sub_gain.reshape(1, VD), w_out)


def to_everyone(value, axis):
    length = lax.axis_size(axis)
    return lax.all_to_all(
        jnp.broadcast_to(value[None], (length, *value.shape)), axis, 0, 0, tiled=True
    )


def body(tokens, w_query, w_key, w_value, w_out, lambda_head, sub_gain):
    tp = lax.axis_size("tp")
    rows = lax.all_gather(tokens, "tp", axis=0, tiled=True)
    dot = functools.partial(lax.dot_general, preferred_element_type=jnp.float32)
    queries = dot(rows, w_query, (((1,), (0,)), ((), ()))).astype(jnp.bfloat16)
    keys = dot(rows, w_key, (((1,), (0,)), ((), ()))).astype(jnp.bfloat16)
    values = dot(w_value, rows, (((0,), (1,)), ((), ()))).astype(jnp.bfloat16)
    all_queries = to_everyone(queries, "y")
    key_values = lax.all_gather(jnp.concatenate([keys, values], axis=0), "z")
    place = jnp.stack([lax.axis_index("z"), lax.axis_index("y")]).astype(jnp.int32)
    parts = attend(place, all_queries, key_values)
    parts = lax.all_to_all(parts, "y", 0, 0, tiled=True)
    partial_rows = merge(parts, lambda_head, sub_gain, w_out)
    arrived = lax.all_to_all(
        partial_rows.reshape(tp, -1, partial_rows.shape[1]), "tp", 0, 0, tiled=True
    )
    return arrived.astype(jnp.float32).sum(axis=0).astype(jnp.bfloat16)


def solution(mesh):
    sp, tp = mesh.devices.shape
    grid = Mesh(mesh.devices.reshape(sp // Y, Y, tp), ("z", "y", "tp"))
    everyone = ("z", "y", "tp")
    return jax.shard_map(
        body,
        mesh=grid,
        in_specs=(
            P(everyone, None),
            P(None, "tp"),
            P(None, "tp"),
            P(None, "tp"),
            P("tp", None),
            P("tp"),
            P(),
        ),
        out_specs=P(everyone, None),
        check_vma=False,
    )
```

```python
import functools
import math

import jax
import jax.numpy as jnp
from jax import lax
from jax.experimental import pallas as pl
from jax.experimental.pallas import tpu as pltpu
from jax.sharding import Mesh, PartitionSpec as P

QK = 64
VD = 128
BLOCK = 128
TILE = 2 * BLOCK
Y = 8
STAT_ROWS = 8
SEND_ROWS = 2 * VD + STAT_ROWS
EMPTY = -1e30
HIDDEN = -2e38
BASE2_SCALE = math.log2(math.e) / math.sqrt(QK)
CASES = ((0, 0, 1), (1, 2, 3), (3, 4, 5), (5, 7, 8), (8, 10, 11), (11, 11, 12))
CHUNK = 2

VMEM = pl.BlockSpec(memory_space=pltpu.VMEM)
SMEM = pl.BlockSpec(memory_space=pltpu.SMEM)


def three_parts(value):
    high = value.astype(jnp.bfloat16)
    rest = value - high.astype(jnp.float32)
    middle = rest.astype(jnp.bfloat16)
    low = (rest - middle.astype(jnp.float32)).astype(jnp.bfloat16)
    return [part.astype(jnp.float32) for part in (high, middle, low)]


def folded(op, value):
    return op(value.reshape(value.shape[0] // 8, 8, value.shape[1]), axis=0)


def both_maps(q_ref, b):
    q_block = q_ref[b]
    q_rows = jnp.concatenate([q_block[:, : 2 * QK], q_block[:, 2 * QK :]], axis=0)
    q_scaled = q_rows.astype(jnp.float32) * BASE2_SCALE
    high = q_scaled.astype(jnp.bfloat16)
    low = (q_scaled - high.astype(jnp.float32)).astype(jnp.bfloat16)
    return [
        jnp.concatenate([high[:, m * QK : (m + 1) * QK], low[:, m * QK : (m + 1) * QK]], axis=1)
        for m in range(2)
    ]


def attend_kernel(place_ref, q_ref, kv_ref, out_ref, v_ref, k0_ref, k1_ref, *scratch):
    z, y = place_ref[0], place_ref[1]
    k_refs = (k0_ref, k1_ref)
    slots = (scratch[0:4], scratch[4:8])
    key_row = lax.broadcasted_iota(jnp.int32, (BLOCK, TILE), 0)
    query_row = lax.rem(lax.broadcasted_iota(jnp.int32, (BLOCK, TILE), 1), BLOCK)
    offsets = key_row - query_row

    def step(case, later, slot_later, now, slot_now, peaks):
        low, _, blocks = case
        pairs_later = [(b, m) for b in later for m in range(2)]
        pairs_now = [(b, m) for b in now for m in range(2)]
        queries = {b: both_maps(q_ref, b) for b in later}
        tops = {p: jnp.full((8, TILE), EMPTY, jnp.float32) for p in pairs_later}
        totals = {p: jnp.zeros((8, TILE), jnp.float32) for p in pairs_now}
        summed = {p: 0.0 for p in pairs_now}
        for first in range(0, blocks, CHUNK):
            last = min(first + CHUNK, blocks)
            rows = slice(first * BLOCK, last * BLOCK)
            for at in range(max(len(pairs_later), len(pairs_now))):
                if at < len(pairs_later):
                    b, m = pairs_later[at]
                    scores = lax.dot_general(
                        k_refs[m][rows, :],
                        queries[b][m],
                        (((1,), (1,)), ((), ())),
                        preferred_element_type=jnp.float32,
                    )
                    for block in range(first, last):
                        part = scores[(block - first) * BLOCK : (block - first + 1) * BLOCK]
                        if block >= low:
                            reach = (z - block) * (Y * BLOCK) + (b - y) * BLOCK
                            part = jnp.where(offsets <= reach, part, HIDDEN)
                        slots[slot_later][at][block * BLOCK : (block + 1) * BLOCK, :] = part
                        tops[b, m] = jnp.maximum(tops[b, m], folded(jnp.max, part))
                if at < len(pairs_now):
                    p = pairs_now[at]
                    expo = jnp.exp2(slots[slot_now][at][rows, :] - peaks[p])
                    totals[p] = totals[p] + folded(jnp.sum, expo)
                    summed[p] = summed[p] + jnp.dot(
                        v_ref[:, rows], expo.astype(jnp.bfloat16), preferred_element_type=jnp.float32
                    )
        for b in now:
            stats = []
            for m in range(2):
                total = jnp.sum(totals[b, m], axis=0, keepdims=True)
                total = total.astype(jnp.bfloat16).astype(jnp.float32)
                inverse = jnp.where(total > 0.0, 1.0 / total, 0.0)
                out_ref[b, m * VD : (m + 1) * VD, :] = (summed[b, m] * inverse).astype(jnp.bfloat16)
                stats += three_parts(peaks[b, m]) + [total]
            out_ref[b, 2 * VD :, :] = jnp.concatenate(stats, axis=0).astype(jnp.bfloat16)
        return {p: jnp.max(top, axis=0, keepdims=True) for p, top in tops.items()}

    for case in CASES:

        @pl.when((z >= case[0]) & (z <= case[1]))
        def _():
            for block in range(case[2]):
                rows = slice(block * BLOCK, (block + 1) * BLOCK)
                v_ref[:, rows] = kv_ref[block, BLOCK:, :]
                k = kv_ref[block, :BLOCK, :]
                k0_ref[rows, :] = jnp.concatenate([k[:, :QK], k[:, :QK]], axis=1)
                k1_ref[rows, :] = jnp.concatenate([k[:, QK:], k[:, QK:]], axis=1)
            turns = [(), *((b, b + 1) for b in range(0, Y, 2)), ()]
            peaks = {}
            for at in range(len(turns) - 1):
                peaks = step(case, turns[at + 1], at % 2, turns[at], (at + 1) % 2, peaks)


def attend(place, queries, key_values):
    span = key_values.shape[0] * BLOCK
    return pl.pallas_call(
        attend_kernel,
        out_shape=jax.ShapeDtypeStruct((Y, SEND_ROWS, TILE), jnp.bfloat16),
        in_specs=[SMEM, VMEM, VMEM],
        out_specs=VMEM,
        scratch_shapes=[pltpu.VMEM((VD, span), jnp.bfloat16)]
        + [pltpu.VMEM((span, 2 * QK), jnp.bfloat16)] * 2
        + [pltpu.VMEM((span, TILE), jnp.float32)] * 8,
        compiler_params=pltpu.CompilerParams(vmem_limit_bytes=22 * 2**20),
        cost_estimate=pl.CostEstimate(
            flops=4_000_000_000, bytes_accessed=3_000_000, transcendentals=6_000_000
        ),
        name="attend",
    )(place, queries, key_values)


def merge_kernel(part_ref, lambda_ref, gain_ref, w_ref, out_ref):
    stats = [part_ref[s, 2 * VD :, :].astype(jnp.float32) for s in range(Y)]
    both = []
    for m in range(2):
        at = 4 * m
        peaks = [s[at : at + 1] + s[at + 1 : at + 2] + s[at + 2 : at + 3] for s in stats]
        totals = [s[at + 3 : at + 4] for s in stats]
        top = functools.reduce(jnp.maximum, peaks)
        shares = [jnp.exp2(p - top) * t for p, t in zip(peaks, totals)]
        inverse = 1.0 / sum(shares)
        both.append(
            sum(
                part_ref[s, m * VD : (m + 1) * VD, :].astype(jnp.float32) * (shares[s] * inverse)
                for s in range(Y)
            )
        )
    column = lax.broadcasted_iota(jnp.int32, (1, TILE), 1)
    mixed = both[0] - jnp.where(column < BLOCK, lambda_ref[0], lambda_ref[1]) * both[1]
    inverse_rms = lax.rsqrt(jnp.mean(mixed * mixed, axis=0, keepdims=True) + 1e-06)
    heads = mixed * inverse_rms
    rows = [heads[:, h * BLOCK : (h + 1) * BLOCK].T * gain_ref[...] for h in range(2)]
    rows = jnp.concatenate(rows, axis=1)
    out_ref[...] = jnp.dot(
        rows.astype(jnp.bfloat16), w_ref[...], preferred_element_type=jnp.float32
    ).astype(jnp.bfloat16)


def merge(parts, lambda_head, sub_gain, w_out):
    return pl.pallas_call(
        merge_kernel,
        out_shape=jax.ShapeDtypeStruct((BLOCK, w_out.shape[1]), jnp.bfloat16),
        in_specs=[VMEM, SMEM, VMEM, VMEM],
        out_specs=VMEM,
        compiler_params=pltpu.CompilerParams(vmem_limit_bytes=12 * 2**20),
        cost_estimate=pl.CostEstimate(
            flops=1_000_000_000, bytes_accessed=3_000_000, transcendentals=8_000
        ),
        name="merge",
    )(parts, lambda_head, sub_gain.reshape(1, VD), w_out)


def to_everyone(value, axis):
    length = lax.axis_size(axis)
    return lax.all_to_all(
        jnp.broadcast_to(value[None], (length, *value.shape)), axis, 0, 0, tiled=True
    )


def body(tokens, w_query, w_key, w_value, w_out, lambda_head, sub_gain):
    tp = lax.axis_size("tp")
    rows = lax.all_gather(tokens, "tp", axis=0, tiled=True)
    dot = functools.partial(lax.dot_general, preferred_element_type=jnp.float32)
    queries = dot(rows, w_query, (((1,), (0,)), ((), ()))).astype(jnp.bfloat16)
    keys = dot(rows, w_key, (((1,), (0,)), ((), ()))).astype(jnp.bfloat16)
    values = dot(w_value, rows, (((0,), (1,)), ((), ()))).astype(jnp.bfloat16)
    all_queries = to_everyone(queries, "y")
    key_values = lax.all_gather(jnp.concatenate([keys, values], axis=0), "z")
    place = jnp.stack([lax.axis_index("z"), lax.axis_index("y")]).astype(jnp.int32)
    parts = attend(place, all_queries, key_values)
    parts = lax.all_to_all(parts, "y", 0, 0, tiled=True)
    partial_rows = merge(parts, lambda_head, sub_gain, w_out)
    arrived = lax.all_to_all(
        partial_rows.reshape(tp, -1, partial_rows.shape[1]), "tp", 0, 0, tiled=True
    )
    return arrived.astype(jnp.float32).sum(axis=0).astype(jnp.bfloat16)


def solution(mesh):
    sp, tp = mesh.devices.shape
    grid = Mesh(mesh.devices.reshape(sp // Y, Y, tp), ("z", "y", "tp"))
    everyone = ("z", "y", "tp")
    return jax.shard_map(
        body,
        mesh=grid,
        in_specs=(
            P(everyone, None),
            P(None, "tp"),
            P(None, "tp"),
            P(None, "tp"),
            P("tp", None),
            P("tp"),
            P(),
        ),
        out_specs=P(everyone, None),
        check_vma=False,
    )
```

```python
import functools
import math

import jax
import jax.numpy as jnp
from jax import lax
from jax.experimental import pallas as pl
from jax.experimental.pallas import tpu as pltpu
from jax.sharding import Mesh, PartitionSpec as P

QK = 64
VD = 128
BLOCK = 128
TILE = 2 * BLOCK
Y = 8
STAT_ROWS = 8
SEND_ROWS = 2 * VD + STAT_ROWS
EMPTY = -1e30
HIDDEN = -2e38
BASE2_SCALE = math.log2(math.e) / math.sqrt(QK)
CASES = ((0, 0, 1), (1, 2, 3), (3, 4, 5), (5, 7, 8), (8, 10, 11), (11, 11, 12))
CHUNK = 2

VMEM = pl.BlockSpec(memory_space=pltpu.VMEM)
SMEM = pl.BlockSpec(memory_space=pltpu.SMEM)


def three_parts(value):
    high = value.astype(jnp.bfloat16)
    rest = value - high.astype(jnp.float32)
    middle = rest.astype(jnp.bfloat16)
    low = (rest - middle.astype(jnp.float32)).astype(jnp.bfloat16)
    return [part.astype(jnp.float32) for part in (high, middle, low)]


def folded(op, value):
    return op(value.reshape(value.shape[0] // 8, 8, value.shape[1]), axis=0)


def both_maps(q_ref, b):
    q_block = q_ref[b]
    q_rows = jnp.concatenate([q_block[:, : 2 * QK], q_block[:, 2 * QK :]], axis=0)
    q_scaled = q_rows.astype(jnp.float32) * BASE2_SCALE
    high = q_scaled.astype(jnp.bfloat16)
    low = (q_scaled - high.astype(jnp.float32)).astype(jnp.bfloat16)
    return [
        jnp.concatenate([high[:, m * QK : (m + 1) * QK], low[:, m * QK : (m + 1) * QK]], axis=1)
        for m in range(2)
    ]


def attend_kernel(place_ref, q_ref, kv_ref, out_ref, v_ref, k0_ref, k1_ref, *scratch):
    z, y = place_ref[0], place_ref[1]
    k_refs = (k0_ref, k1_ref)
    slots = (scratch[0:4], scratch[4:8])
    key_row = lax.broadcasted_iota(jnp.int32, (BLOCK, TILE), 0)
    query_row = lax.rem(lax.broadcasted_iota(jnp.int32, (BLOCK, TILE), 1), BLOCK)
    offsets = key_row - query_row

    def step(case, later, slot_later, now, slot_now, peaks):
        low, _, blocks = case
        pairs_later = [(b, m) for b in later for m in range(2)]
        pairs_now = [(b, m) for b in now for m in range(2)]
        queries = {b: both_maps(q_ref, b) for b in later}
        tops = {p: jnp.full((8, TILE), EMPTY, jnp.float32) for p in pairs_later}
        totals = {p: jnp.zeros((8, TILE), jnp.float32) for p in pairs_now}
        summed = {p: 0.0 for p in pairs_now}
        for first in range(0, blocks, CHUNK):
            last = min(first + CHUNK, blocks)
            rows = slice(first * BLOCK, last * BLOCK)
            for at in range(max(len(pairs_later), len(pairs_now))):
                if at < len(pairs_later):
                    b, m = pairs_later[at]
                    scores = lax.dot_general(
                        k_refs[m][rows, :],
                        queries[b][m],
                        (((1,), (1,)), ((), ())),
                        preferred_element_type=jnp.float32,
                    )
                    for block in range(first, last):
                        part = scores[(block - first) * BLOCK : (block - first + 1) * BLOCK]
                        if block >= low:
                            reach = (z - block) * (Y * BLOCK) + (b - y) * BLOCK
                            part = jnp.where(offsets <= reach, part, HIDDEN)
                        slots[slot_later][at][block * BLOCK : (block + 1) * BLOCK, :] = part
                        tops[b, m] = jnp.maximum(tops[b, m], folded(jnp.max, part))
                if at < len(pairs_now):
                    p = pairs_now[at]
                    expo = jnp.exp2(slots[slot_now][at][rows, :] - peaks[p])
                    totals[p] = totals[p] + folded(jnp.sum, expo)
                    summed[p] = summed[p] + jnp.dot(
                        v_ref[:, rows], expo.astype(jnp.bfloat16), preferred_element_type=jnp.float32
                    )
        for b in now:
            stats = []
            for m in range(2):
                total = jnp.sum(totals[b, m], axis=0, keepdims=True)
                total = total.astype(jnp.bfloat16).astype(jnp.float32)
                inverse = jnp.where(total > 0.0, 1.0 / total, 0.0)
                out_ref[b, m * VD : (m + 1) * VD, :] = (summed[b, m] * inverse).astype(jnp.bfloat16)
                stats += three_parts(peaks[b, m]) + [total]
            out_ref[b, 2 * VD :, :] = jnp.concatenate(stats, axis=0).astype(jnp.bfloat16)
        return {p: jnp.max(top, axis=0, keepdims=True) for p, top in tops.items()}

    for case in CASES:

        @pl.when((z >= case[0]) & (z <= case[1]))
        def _():
            for block in range(case[2]):
                rows = slice(block * BLOCK, (block + 1) * BLOCK)
                v_ref[:, rows] = kv_ref[block, BLOCK:, :]
                k = kv_ref[block, :BLOCK, :]
                k0_ref[rows, :] = jnp.concatenate([k[:, :QK], k[:, :QK]], axis=1)
                k1_ref[rows, :] = jnp.concatenate([k[:, QK:], k[:, QK:]], axis=1)
            turns = [(), *((b, b + 1) for b in range(0, Y, 2)), ()]
            peaks = {}
            for at in range(len(turns) - 1):
                peaks = step(case, turns[at + 1], at % 2, turns[at], (at + 1) % 2, peaks)


def attend(place, queries, key_values):
    span = key_values.shape[0] * BLOCK
    return pl.pallas_call(
        attend_kernel,
        out_shape=jax.ShapeDtypeStruct((Y, SEND_ROWS, TILE), jnp.bfloat16),
        in_specs=[SMEM, VMEM, VMEM],
        out_specs=VMEM,
        scratch_shapes=[pltpu.VMEM((VD, span), jnp.bfloat16)]
        + [pltpu.VMEM((span, 2 * QK), jnp.bfloat16)] * 2
        + [pltpu.VMEM((span, TILE), jnp.float32)] * 8,
        compiler_params=pltpu.CompilerParams(vmem_limit_bytes=22 * 2**20),
        cost_estimate=pl.CostEstimate(
            flops=4_000_000_000, bytes_accessed=3_000_000, transcendentals=6_000_000
        ),
        name="attend",
    )(place, queries, key_values)


def merge_kernel(part_ref, lambda_ref, gain_ref, w_ref, out_ref):
    stats = [part_ref[s, 2 * VD :, :].astype(jnp.float32) for s in range(Y)]
    both = []
    for m in range(2):
        at = 4 * m
        peaks = [s[at : at + 1] + s[at + 1 : at + 2] + s[at + 2 : at + 3] for s in stats]
        totals = [s[at + 3 : at + 4] for s in stats]
        top = functools.reduce(jnp.maximum, peaks)
        shares = [jnp.exp2(p - top) * t for p, t in zip(peaks, totals)]
        inverse = 1.0 / sum(shares)
        both.append(
            sum(
                part_ref[s, m * VD : (m + 1) * VD, :].astype(jnp.float32) * (shares[s] * inverse)
                for s in range(Y)
            )
        )
    column = lax.broadcasted_iota(jnp.int32, (1, TILE), 1)
    mixed = both[0] - jnp.where(column < BLOCK, lambda_ref[0], lambda_ref[1]) * both[1]
    inverse_rms = lax.rsqrt(jnp.mean(mixed * mixed, axis=0, keepdims=True) + 1e-06)
    heads = mixed * inverse_rms
    rows = [heads[:, h * BLOCK : (h + 1) * BLOCK].T * gain_ref[...] for h in range(2)]
    rows = jnp.concatenate(rows, axis=1)
    out_ref[...] = jnp.dot(
        rows.astype(jnp.bfloat16), w_ref[...], preferred_element_type=jnp.float32
    ).astype(jnp.bfloat16)


def merge(parts, lambda_head, sub_gain, w_out):
    return pl.pallas_call(
        merge_kernel,
        out_shape=jax.ShapeDtypeStruct((BLOCK, w_out.shape[1]), jnp.bfloat16),
        in_specs=[VMEM, SMEM, VMEM, VMEM],
        out_specs=VMEM,
        compiler_params=pltpu.CompilerParams(vmem_limit_bytes=12 * 2**20),
        cost_estimate=pl.CostEstimate(
            flops=1_000_000_000, bytes_accessed=3_000_000, transcendentals=8_000
        ),
        name="merge",
    )(parts, lambda_head, sub_gain.reshape(1, VD), w_out)


def sum_kernel(part_ref, out_ref):
    total = part_ref[0].astype(jnp.float32)
    for n in range(1, part_ref.shape[0]):
        total = total + part_ref[n].astype(jnp.float32)
    out_ref[...] = total.astype(jnp.bfloat16)


def summed_rows(parts):
    return pl.pallas_call(
        sum_kernel,
        out_shape=jax.ShapeDtypeStruct(parts.shape[1:], jnp.bfloat16),
        in_specs=[VMEM],
        out_specs=VMEM,
        compiler_params=pltpu.CompilerParams(vmem_limit_bytes=4 * 2**20),
        name="sum_rows",
    )(parts)


def to_everyone(value, axis):
    length = lax.axis_size(axis)
    return lax.all_to_all(
        jnp.broadcast_to(value[None], (length, *value.shape)), axis, 0, 0, tiled=True
    )


def body(tokens, w_query, w_key, w_value, w_out, lambda_head, sub_gain):
    tp = lax.axis_size("tp")
    rows = lax.all_gather(tokens, "tp", axis=0, tiled=True)
    dot = functools.partial(lax.dot_general, preferred_element_type=jnp.float32)
    queries = dot(rows, w_query, (((1,), (0,)), ((), ()))).astype(jnp.bfloat16)
    keys = dot(rows, w_key, (((1,), (0,)), ((), ()))).astype(jnp.bfloat16)
    values = dot(w_value, rows, (((0,), (1,)), ((), ()))).astype(jnp.bfloat16)
    all_queries = to_everyone(queries, "y")
    key_values = lax.all_gather(jnp.concatenate([keys, values], axis=0), "z")
    place = jnp.stack([lax.axis_index("z"), lax.axis_index("y")]).astype(jnp.int32)
    parts = attend(place, all_queries, key_values)
    parts = lax.all_to_all(parts, "y", 0, 0, tiled=True)
    partial_rows = merge(parts, lambda_head, sub_gain, w_out)
    arrived = lax.all_to_all(
        partial_rows.reshape(tp, -1, partial_rows.shape[1]), "tp", 0, 0, tiled=True
    )
    return summed_rows(arrived)


def solution(mesh):
    sp, tp = mesh.devices.shape
    grid = Mesh(mesh.devices.reshape(sp // Y, Y, tp), ("z", "y", "tp"))
    everyone = ("z", "y", "tp")
    return jax.shard_map(
        body,
        mesh=grid,
        in_specs=(
            P(everyone, None),
            P(None, "tp"),
            P(None, "tp"),
            P(None, "tp"),
            P("tp", None),
            P("tp"),
            P(),
        ),
        out_specs=P(everyone, None),
        check_vma=False,
    )
```
